32 devices in a mesh: fs: 8 (over z, x), tp: 4 (over y, core).
Axes of the slice: x: 2, y: 2, z: 4, core: 2. Of those that a mesh axis runs over, the one named last changes fastest.
Arguments:
- tokens: bfloat16 [1536, 2048], P('fs'), may hold values from -6 to 6
- norm_gain: float32 [2048], P('fs'), may hold values from 0.1 to 1.9
- expert_gate: float32 [16, 2048, 1024], P(None, 'fs', 'tp'), may hold values from -0.125 to 0.125
- expert_up: float32 [16, 2048, 1024], P(None, 'fs', 'tp'), may hold values from -0.125 to 0.125
- expert_down: float32 [16, 1024, 2048], P(None, 'fs', 'tp'), may hold values from -0.1875 to 0.1875
- shared_gate: float32 [2048, 1024], P('fs', 'tp'), may hold values from -0.125 to 0.125
- shared_up: float32 [2048, 1024], P('fs', 'tp'), may hold values from -0.125 to 0.125
- shared_down: float32 [1024, 2048], P('fs', 'tp'), may hold values from -0.1875 to 0.1875
- expert_ids: int32 [1536, 8], P('fs'), may hold values from 0 to 15, all different within a row; in each aligned block of 192 rows (0 to 191, 192 to 383, ...) at most 192 rows name the same one
- route_weights: float32 [1536, 8], P('fs'), may hold values from 0.25 to 1
Outputs:
- gate_ready: bfloat16 [16, 2048, 1024], P('fs', None, 'tp')
- up_ready: bfloat16 [16, 2048, 1024], P('fs', None, 'tp')
- down_ready: bfloat16 [16, 1024, 2048], P('fs', None, 'tp')
- shared_gate_ready: bfloat16 [2048, 1024], P(None, 'tp')
- shared_up_ready: bfloat16 [2048, 1024], P(None, 'tp')
- shared_down_ready: bfloat16 [1024, 2048], P(None, 'tp')
- mixed: bfloat16 [1536, 2048], P('fs', 'tp')
The draws below stay inside these ranges and needn't reach their ends.
Inputs may be any that keep to these rules, and one draw needn't show every extreme that they name: `expert_ids`: each row names 8 different experts. Among the 192 rows of one index of fs no expert is named more than 192 times, and in every draw some expert is named exactly 192 times there.
All inputs are finite; a program needn't handle non-finite values.
Results may differ from the reference program's by a relative error of at most 0.0085.
Values may be sent and summed in bfloat16 or wider, within the bound.
No kernel may reach another device: no remote copies, remote signals or barrier semaphores. Data moves between devices by JAX's collectives and lax.ppermute only.
A program may use at most 128 MiB of HBM per device.

```python
import math
import jax
import jax.numpy as jnp
import numpy as np
from jax import lax

D = 2048
DE = 1024
TOP_K = 8
TOK_DEV = 192
EXPERTS = 16
TOKENS = 1536
CAPE = 192
N_FS = 8


def steps_of(own_key, extent, pieces, low, top_value):
    level, own = 1.0, jax.random.fold_in(own_key, 6)
    for axis_at, parts in pieces:
        draws = jnp.exp(jax.random.uniform(jax.random.fold_in(own, axis_at), (parts,), jnp.float32, low / len(pieces), top_value / len(pieces)))
        level = level * jnp.repeat(draws, extent[axis_at] // parts).reshape([-1 if axis == axis_at else 1 for axis in range(len(extent))])
    return level


def routed_block(key, own, number, rows, count, top, limit, slope):
    ranking = jax.random.permutation(key, count)
    crowded, common = shares(count, rows * top, limit, slope, True), shares(count, rows * top, limit, slope, False)
    places = jnp.arange(count)

    def named(tallies, offset_by):
        used = int((tallies > 0).sum())
        fixed = max(1, used // 4)
        moved = fixed + (places - fixed + offset_by * (used - fixed)) % max(1, count - fixed)
        return jnp.zeros((count,), jnp.int32).at[ranking[jnp.where(places < fixed, places, moved)]].set(jnp.asarray(tallies, jnp.int32))

    tallies = jnp.where(number % 4 == 0, named(crowded, number // 4), named(common, number - number // 4 - 1))
    mixed = jax.random.permutation(jax.random.fold_in(own, 3), count)
    giver, receiver = mixed[0:count // 2 * 2:2], mixed[1:count // 2 * 2:2]
    slack = jnp.minimum(tallies[giver] - 1, limit - tallies[receiver]) // 2
    slack = jnp.where((giver == ranking[0]) | (receiver == ranking[0]) | (tallies[receiver] == 0), 0, jnp.maximum(slack, 0))
    moved = jax.random.randint(jax.random.fold_in(own, 4), (count // 2,), 0, 1 << 20) % (slack + 1)
    tallies = tallies.at[giver].add(-moved).at[receiver].add(moved)
    members = jnp.searchsorted(jnp.cumsum(tallies), jnp.arange(rows * top), side="right").astype(jnp.int32)
    grid = members.reshape(top, rows).T
    grid = grid[jax.random.permutation(jax.random.fold_in(own, 1), rows)]
    offset_by = jax.random.randint(jax.random.fold_in(own, 2), (rows, 1), 0, top)
    return jnp.take_along_axis(grid, (jnp.arange(top)[None, :] + offset_by) % top, axis=1)


def shares(count, total, bound, lean, full):
    portions = [(1 << 20) // math.isqrt(rank ** lean) + 1 for rank in range(1, count + 1)]
    largest = bound if full else min(bound, max(-(-total // count), total * portions[0] // sum(portions)))
    least = 1 if total - largest >= count - 1 else 0
    counts, spare = [largest] + [least] * (count - 1), total - largest - least * (count - 1)
    while spare > 0:
        candidates = [i for i in range(1, count) if counts[i] < largest] or [i for i in range(1, count) if counts[i] < bound]
        pool, remaining = sum([portions[i] for i in candidates]), spare
        for i in candidates:
            more = min(bound - counts[i], max(1, remaining * portions[i] // pool), spare)
            counts[i] = counts[i] + more
            spare = spare - more
    return np.array(counts)


def scatter_about(own_key, dims, spread, reach, cuts=(), kind=jnp.bfloat16):
    values = spread * jax.random.normal(own_key, dims, jnp.float32)
    if cuts:
        values = values * steps_of(own_key, dims, cuts, -0.22, 0.18)
    return jnp.clip(values, -reach, reach).astype(kind)


def setup_inputs(seed: int = 0) -> dict:
    arg_keys = jax.random.split(jax.random.key(seed), 11)
    tokens = scatter_about(arg_keys[0], (TOKENS, D), 1.0, 6.0, ((0, 8),))
    norm_gain = jnp.clip(1.0 + 0.18 * jax.random.normal(arg_keys[1], (D,), jnp.float32), 0.1, 1.9)
    expert_gate = scatter_about(arg_keys[2], (EXPERTS, D, DE), D ** -0.5, 0.125, ((1, 8), (2, 4)), jnp.float32)
    expert_up = scatter_about(arg_keys[3], (EXPERTS, D, DE), D ** -0.5, 0.125, ((1, 8), (2, 4)), jnp.float32)
    expert_down = scatter_about(arg_keys[4], (EXPERTS, DE, D), DE ** -0.5, 0.1875, ((1, 8), (2, 4)), jnp.float32)
    shared_gate = scatter_about(arg_keys[5], (D, DE), D ** -0.5, 0.125, ((0, 8), (1, 4)), jnp.float32)
    shared_up = scatter_about(arg_keys[6], (D, DE), D ** -0.5, 0.125, ((0, 8), (1, 4)), jnp.float32)
    shared_down = scatter_about(arg_keys[7], (DE, D), DE ** -0.5, 0.1875, ((0, 8), (1, 4)), jnp.float32)
    expert_ids_keys = jax.random.split(jax.random.fold_in(arg_keys[8], 1), TOKENS // TOK_DEV)
    expert_ids_turns = jax.random.permutation(jax.random.fold_in(arg_keys[8], 3), TOKENS // TOK_DEV)
    expert_ids = jax.vmap(lambda own, number: routed_block(jax.random.fold_in(arg_keys[8], 2), own, number, TOK_DEV, EXPERTS, TOP_K, CAPE, 1))(expert_ids_keys, expert_ids_turns).reshape((TOKENS, TOP_K))
    route_weights = jnp.clip(jnp.exp(math.log(1.0) - 1.3862944 * jax.random.uniform(arg_keys[9], (TOKENS, TOP_K), jnp.float32) ** steps_of(arg_keys[9], (TOKENS, TOP_K), ((0, 8),), -0.2, 0.2)), 0.25, 1.0)
    return {"tokens": tokens, "norm_gain": norm_gain, "expert_gate": expert_gate, "expert_up": expert_up, "expert_down": expert_down, "shared_gate": shared_gate, "shared_up": shared_up, "shared_down": shared_down, "expert_ids": expert_ids, "route_weights": route_weights}


EPS = 1e-06

def reference(tokens, norm_gain, expert_gate, expert_up, expert_down, shared_gate, shared_up, shared_down, expert_ids, route_weights):
    gain = norm_gain.astype(jnp.float32)
    gate_ready = (expert_gate * gain[None, :, None]).astype(jnp.bfloat16)
    up_ready = (expert_up * gain[None, :, None]).astype(jnp.bfloat16)
    down_ready = expert_down.astype(jnp.bfloat16)
    shared_gate_ready = (shared_gate * gain[:, None]).astype(jnp.bfloat16)
    shared_up_ready = (shared_up * gain[:, None]).astype(jnp.bfloat16)
    shared_down_ready = shared_down.astype(jnp.bfloat16)
    wide = tokens.astype(jnp.float32)
    normed = (wide * lax.rsqrt(lax.optimization_barrier(jnp.mean(wide * wide, axis=-1, keepdims=True)) + EPS)).astype(jnp.bfloat16)
    shared_first = jnp.dot(normed, shared_gate_ready, preferred_element_type=jnp.float32)
    shared_second = jnp.dot(normed, shared_up_ready, preferred_element_type=jnp.float32)
    shared_hidden = (jax.nn.silu(shared_first) * shared_second).astype(jnp.bfloat16)
    shared_out = jnp.dot(shared_hidden, shared_down_ready, preferred_element_type=jnp.float32)
    experts = expert_gate.shape[0]
    tok_block = tokens.shape[0] // N_FS
    capacity = 2 * tok_block * TOP_K // experts
    chosen = expert_ids.reshape(N_FS, tok_block * TOP_K).astype(jnp.int32)
    onehot = (chosen[..., None] == jnp.arange(experts, dtype=jnp.int32)).astype(jnp.int32)
    ranks = (lax.optimization_barrier(jnp.sum(jnp.cumsum(onehot, axis=1) * onehot, axis=-1)) - 1).astype(jnp.int32)
    blocks = jnp.broadcast_to(jnp.arange(N_FS, dtype=jnp.int32)[:, None], chosen.shape)
    owners = (blocks * tok_block + jnp.arange(tok_block * TOP_K, dtype=jnp.int32)[None, :] // TOP_K).astype(jnp.int32)
    slot_token = jnp.zeros((experts, N_FS, capacity), jnp.int32).at[chosen, blocks, ranks].set(owners)
    slot_weight = jnp.zeros((experts, N_FS, capacity), jnp.float32).at[chosen, blocks, ranks].set(route_weights.reshape(N_FS, -1).astype(jnp.float32))

    def one_expert(total, index):
        which = slot_token[index].reshape(-1)
        rows = normed[which]
        first = jnp.dot(rows, gate_ready[index], preferred_element_type=jnp.float32)
        second = jnp.dot(rows, up_ready[index], preferred_element_type=jnp.float32)
        hidden = (jax.nn.silu(first) * second).astype(jnp.bfloat16)
        result = jnp.dot(hidden, down_ready[index], preferred_element_type=jnp.float32).astype(jnp.bfloat16)
        result = lax.optimization_barrier(result).astype(jnp.float32)
        return (total.at[which].add(result * slot_weight[index].reshape(-1)[:, None]), None)
    routed, _ = lax.scan(one_expert, jnp.zeros(tokens.shape, jnp.float32), jnp.arange(experts, dtype=jnp.int32))
    mixed = (shared_out + routed).astype(jnp.bfloat16)
    return (gate_ready, up_ready, down_ready, shared_gate_ready, shared_up_ready, shared_down_ready, mixed)
```

```python
import jax
import jax.numpy as jnp
from jax import lax
from jax.sharding import PartitionSpec as P


EPS = 1e-06
LANES = 128


def layer(
    tokens,
    norm_gain,
    expert_gate,
    expert_up,
    expert_down,
    shared_gate,
    shared_up,
    shared_down,
    expert_ids,
    route_weights,
):
    groups = lax.axis_size("fs")
    tp = lax.axis_size("tp")
    experts = expert_gate.shape[0]
    per_group = experts // groups
    tok_count, width = tokens.shape
    bf16, f32 = jnp.bfloat16, jnp.float32

    wide = tokens.astype(f32)
    normed = (wide * lax.rsqrt(jnp.mean(wide * wide, axis=-1, keepdims=True) + EPS)).astype(bf16)
    chosen = expert_ids[:, :, None] == jnp.arange(experts, dtype=jnp.int32)[None, None, :]
    dense = jnp.sum(jnp.where(chosen, route_weights[:, :, None], 0.0), axis=1)
    high = lax.reduce_precision(dense, 8, 7)
    low = (dense - high).astype(bf16)
    columns = jnp.concatenate([high.astype(bf16), low], axis=1)
    columns = jnp.pad(columns, ((0, 0), (0, -columns.shape[1] % LANES)))
    share = tok_count // tp
    rows = jnp.concatenate([normed, columns], axis=1)
    mine = lax.dynamic_slice_in_dim(rows, lax.axis_index("tp") * share, share, 0)
    everyone = lax.all_gather(mine, ("fs", "tp"), axis=0, tiled=True)
    all_tokens = everyone[:, :width]
    own = lax.axis_index("fs") * per_group
    weight = lax.dynamic_slice_in_dim(
        everyone[:, width : width + experts].astype(f32)
        + everyone[:, width + experts : width + 2 * experts].astype(f32),
        own,
        per_group,
        1,
    )

    sg = (shared_gate * norm_gain[:, None]).astype(bf16)
    su = (shared_up * norm_gain[:, None]).astype(bf16)
    sd = shared_down.astype(bf16)
    part = sg.shape[1]
    stacked = jnp.concatenate([jnp.concatenate([sg, su], axis=1), sd], axis=0)
    gathered = lax.all_gather(stacked, "fs", axis=0)
    head = sg.shape[0]
    shared_gate_ready = gathered[:, :head, :part].reshape(groups * head, part)
    shared_up_ready = gathered[:, :head, part:].reshape(groups * head, part)
    shared_down_ready = gathered[:, head:, :].reshape(groups * sd.shape[0], sd.shape[1])

    def moved(local):
        local = local.reshape((groups, per_group) + local.shape[1:])
        return lax.all_to_all(local, "fs", split_axis=0, concat_axis=2, tiled=True)[0]

    gate_ready = moved((expert_gate * norm_gain[None, :, None]).astype(bf16))
    up_ready = moved((expert_up * norm_gain[None, :, None]).astype(bf16))
    down_ready = moved(expert_down.astype(bf16))

    first = jnp.einsum("td,edf->etf", all_tokens, gate_ready, preferred_element_type=f32)
    second = jnp.einsum("td,edf->etf", all_tokens, up_ready, preferred_element_type=f32)
    hidden = (jax.nn.silu(first) * second * weight.T[:, :, None]).astype(bf16)
    routed_hidden = lax.all_gather(hidden, "tp", axis=2, tiled=True)
    partial = jnp.einsum("etf,efd->td", routed_hidden, down_ready, preferred_element_type=f32)
    partial = partial.astype(bf16).reshape(groups, tok_count, partial.shape[1])
    returned = lax.all_to_all(partial, "fs", split_axis=0, concat_axis=0, tiled=True)

    shared_first = jnp.dot(normed, shared_gate_ready, preferred_element_type=f32)
    shared_second = jnp.dot(normed, shared_up_ready, preferred_element_type=f32)
    shared_hidden = (jax.nn.silu(shared_first) * shared_second).astype(bf16)
    shared_piece = lax.all_gather(shared_hidden, "tp", axis=1, tiled=True)
    shared_total = jnp.dot(shared_piece, shared_down_ready, preferred_element_type=f32)
    mixed = (shared_total + jnp.sum(returned.astype(f32), axis=0)).astype(bf16)
    return (
        gate_ready,
        up_ready,
        down_ready,
        shared_gate_ready,
        shared_up_ready,
        shared_down_ready,
        mixed,
    )


def solution(mesh):
    in_specs = (
        P("fs", None),
        P("fs"),
        P(None, "fs", "tp"),
        P(None, "fs", "tp"),
        P(None, "fs", "tp"),
        P("fs", "tp"),
        P("fs", "tp"),
        P("fs", "tp"),
        P("fs", None),
        P("fs", None),
    )
    out_specs = (
        P("fs", None, "tp"),
        P("fs", None, "tp"),
        P("fs", None, "tp"),
        P(None, "tp"),
        P(None, "tp"),
        P(None, "tp"),
        P("fs", "tp"),
    )
    return jax.shard_map(layer, mesh=mesh, in_specs=in_specs, out_specs=out_specs, check_vma=False)
```

```python
import jax
import jax.numpy as jnp
from jax import lax
from jax.sharding import PartitionSpec as P


EPS = 1e-06
LANES = 128


def layer(
    tokens,
    norm_gain,
    expert_gate,
    expert_up,
    expert_down,
    shared_gate,
    shared_up,
    shared_down,
    expert_ids,
    route_weights,
):
    groups = lax.axis_size("fs")
    tp = lax.axis_size("tp")
    experts = expert_gate.shape[0]
    per_group = experts // groups
    tok_count, width = tokens.shape
    bf16, f32 = jnp.bfloat16, jnp.float32

    def normalised(block):
        wide = block.astype(f32)
        scale = lax.rsqrt(jnp.mean(wide * wide, axis=-1, keepdims=True) + EPS)
        return (wide * scale).astype(bf16)

    chosen = expert_ids[:, :, None] == jnp.arange(experts, dtype=jnp.int32)[None, None, :]
    dense = jnp.sum(jnp.where(chosen, route_weights[:, :, None], 0.0), axis=1)
    high = lax.reduce_precision(dense, 8, 7)
    low = (dense - high).astype(bf16)
    columns = jnp.concatenate([high.astype(bf16), low], axis=1)
    columns = jnp.pad(columns, ((0, 0), (0, -columns.shape[1] % LANES)))
    share = tok_count // tp
    rows = jnp.concatenate([tokens, columns], axis=1)
    mine = lax.dynamic_slice_in_dim(rows, lax.axis_index("tp") * share, share, 0)
    mine = lax.all_gather(mine, "fs", axis=0)
    mine = jnp.concatenate([normalised(mine[:, :, :width]), mine[:, :, width:]], axis=2)
    everyone = lax.all_gather(mine, "tp", axis=1, tiled=True)
    everyone = everyone.reshape(groups * tok_count, everyone.shape[2])
    all_tokens = everyone[:, :width]
    own = lax.axis_index("fs") * per_group
    line = jnp.arange(everyone.shape[1] - width, dtype=jnp.int32)[:, None]
    target = own + jnp.arange(per_group, dtype=jnp.int32)[None, :]
    pick = ((line == target) | (line == target + experts)).astype(bf16)
    weight = jnp.einsum("tc,ce->et", everyone[:, width:], pick, preferred_element_type=f32)

    sg = (shared_gate * norm_gain[:, None]).astype(bf16)
    su = (shared_up * norm_gain[:, None]).astype(bf16)
    sd = shared_down.astype(bf16)
    part = sg.shape[1]
    gathered = lax.all_gather(jnp.concatenate([sg, su], axis=1), "fs", axis=0, tiled=True)
    shared_down_ready = lax.all_gather(sd, "fs", axis=0, tiled=True)
    shared_gate_ready = gathered[:, :part]
    shared_up_ready = gathered[:, part:]

    def moved(local):
        local = local.reshape((groups, per_group) + local.shape[1:])
        return lax.all_to_all(local, "fs", split_axis=0, concat_axis=0, tiled=True)

    def ready(block):
        return block.transpose(1, 0, 2, 3).reshape(per_group, -1, block.shape[3])

    def of(block, e):
        return block[:, e].reshape(-1, block.shape[3])

    gate_local = (expert_gate * norm_gain[None, :, None]).astype(bf16)
    gate_local, expert_up = lax.optimization_barrier((gate_local, expert_up))
    gate_moved = moved(gate_local)
    up_local = (expert_up * norm_gain[None, :, None]).astype(bf16)
    up_moved = moved(up_local)
    down_moved = moved(expert_down.astype(bf16))
    gate_ready, up_ready, down_ready = ready(gate_moved), ready(up_moved), ready(down_moved)

    total = 0.0
    for e in range(per_group):
        gate_e, up_e = of(gate_moved, e), of(up_moved, e)
        first = jnp.dot(all_tokens, gate_e, preferred_element_type=f32)
        second = jnp.dot(all_tokens, up_e, preferred_element_type=f32)
        hidden = (jax.nn.silu(first) * second * weight[e][:, None]).astype(bf16)
        spread = lax.all_gather(hidden, "tp", axis=1, tiled=True)
        total = total + jnp.dot(spread, of(down_moved, e), preferred_element_type=f32)
    partial = total.astype(bf16).reshape(groups, tok_count, total.shape[1])
    returned = lax.all_to_all(partial, "fs", split_axis=0, concat_axis=0, tiled=True)
    returned = jnp.sum(returned.astype(f32), axis=0)

    normed = normalised(tokens)
    shared_first = jnp.dot(normed, shared_gate_ready, preferred_element_type=f32)
    shared_second = jnp.dot(normed, shared_up_ready, preferred_element_type=f32)
    shared_hidden = (jax.nn.silu(shared_first) * shared_second).astype(bf16)
    shared_piece = lax.all_gather(shared_hidden, "tp", axis=1, tiled=True)
    shared_total = jnp.dot(shared_piece, shared_down_ready, preferred_element_type=f32)
    mixed = (shared_total + returned).astype(bf16)
    return (
        gate_ready,
        up_ready,
        down_ready,
        shared_gate_ready,
        shared_up_ready,
        shared_down_ready,
        mixed,
    )


def solution(mesh):
    in_specs = (
        P("fs", None),
        P("fs"),
        P(None, "fs", "tp"),
        P(None, "fs", "tp"),
        P(None, "fs", "tp"),
        P("fs", "tp"),
        P("fs", "tp"),
        P("fs", "tp"),
        P("fs", None),
        P("fs", None),
    )
    out_specs = (
        P("fs", None, "tp"),
        P("fs", None, "tp"),
        P("fs", None, "tp"),
        P(None, "tp"),
        P(None, "tp"),
        P(None, "tp"),
        P("fs", "tp"),
    )
    return jax.shard_map(layer, mesh=mesh, in_specs=in_specs, out_specs=out_specs, check_vma=False)
```
